32 devices in a mesh: ep: 4 (over z), tp: 8 (over y, x, core).
Axes of the slice: x: 2, y: 2, z: 4, core: 2. Of those that a mesh axis runs over, the one named last changes fastest.
Arguments:
- tokens: bfloat16 [4096, 2048], P(('ep', 'tp')), may hold values from -40 to 40
- norm_gain: float32 [2048], replicated, may hold values from 0.1 to 1.9
- routes: int32 [4096, 2], P(('ep', 'tp')), may hold values from 0 to 7, all different within a row; in each aligned block of 128 rows (0 to 127, 128 to 255, ...) at most 64 rows name the same one
- gates: float32 [4096, 2], P(('ep', 'tp')), may hold values from 0.25 to 2
- expert_gate: bfloat16 [8, 2048, 512], P('tp'), may hold values from -0.125 to 0.125
- expert_up: bfloat16 [8, 2048, 512], P('tp'), may hold values from -0.125 to 0.125
- expert_down: bfloat16 [8, 512, 2048], P('tp'), may hold values from -0.25 to 0.25
- shared_gate: bfloat16 [2048, 256], replicated, may hold values from -0.125 to 0.125
- shared_up: bfloat16 [2048, 256], replicated, may hold values from -0.125 to 0.125
- shared_down: bfloat16 [256, 2048], replicated, may hold values from -0.375 to 0.375
Outputs:
- mixed: bfloat16 [4096, 2048], P(('ep', 'tp'))
- load: float32 [8], replicated
The draws below stay inside these ranges and needn't reach their ends.
Inputs may be any that keep to these rules, and one draw needn't show every extreme that they name: `routes`: each row names 2 different experts. Among the rows of one device no expert is named by more than 64 rows, and in every draw some expert is named by exactly 64 rows of some device.
All inputs are finite; a program needn't handle non-finite values.
Results may differ from the reference program's by a relative error of at most 0.002.
The reference program's roundings to bfloat16 on the way count: a program that leaves them out, or rounds other values in their place, can miss the bound.
Values may be sent and summed in bfloat16 or wider, within the bound.
A program may use at most 64 MiB of HBM per device.

```python
import math
import jax
import jax.numpy as jnp
import numpy as np
from jax import lax

D = 2048
EXPERT_UNITS = 512
SHARED = 256
TOPK = 2
TOK_DEV = 128
EXPERTS = 8
CAP = 64
TOKENS = 4096


def draw_tokens(key, part):
    key_values, key_column, key_row = jax.random.split(key, 3)
    column_scale = jnp.exp(jax.random.uniform(key_column, (D,), jnp.float32, jnp.log(0.5), jnp.log(5.0)))
    row_scale = jnp.exp(jax.random.uniform(key_row, (TOKENS, 1), jnp.float32, jnp.log(0.5), jnp.log(2.0)))
    base_values = jnp.clip(jax.random.normal(key_values, (TOKENS, D), jnp.float32), -4.0, 4.0)
    return (base_values * column_scale * row_scale).astype(jnp.bfloat16)


def level_of(stream_key, shape, pieces, low, high):
    level, own = 1.0, jax.random.fold_in(stream_key, 6)
    for axis_at, parts in pieces:
        heights = jnp.exp(jax.random.uniform(jax.random.fold_in(own, axis_at), (parts,), jnp.float32, low / len(pieces), high / len(pieces)))
        level = level * jnp.repeat(heights, shape[axis_at] // parts).reshape([-1 if axis == axis_at else 1 for axis in range(len(shape))])
    return level


def routed_block(own_key, own, number, rows, number_of, top, bound, skew):
    ranking = jax.random.permutation(own_key, number_of)
    crowded, ordinary = load_shares(number_of, rows * top, bound, skew, True), load_shares(number_of, rows * top, bound, skew, False)
    places = jnp.arange(number_of)

    def named(lengths, rotation):
        used = int((lengths > 0).sum())
        fixed = max(1, used // 4)
        passed = fixed + (places - fixed + rotation * (used - fixed)) % max(1, number_of - fixed)
        return jnp.zeros((number_of,), jnp.int32).at[ranking[jnp.where(places < fixed, places, passed)]].set(jnp.asarray(lengths, jnp.int32))

    lengths = jnp.where(number % 4 == 0, named(crowded, number // 4), named(ordinary, number - number // 4 - 1))
    mixed = jax.random.permutation(jax.random.fold_in(own, 3), number_of)
    donor, sink = mixed[0:number_of // 2 * 2:2], mixed[1:number_of // 2 * 2:2]
    slack = jnp.minimum(lengths[donor] - 1, bound - lengths[sink]) // 2
    slack = jnp.where((donor == ranking[0]) | (sink == ranking[0]) | (lengths[sink] == 0), 0, jnp.maximum(slack, 0))
    passed = jax.random.randint(jax.random.fold_in(own, 4), (number_of // 2,), 0, 1 << 20) % (slack + 1)
    lengths = lengths.at[donor].add(-passed).at[sink].add(passed)
    items = jnp.searchsorted(jnp.cumsum(lengths), jnp.arange(rows * top), side="right").astype(jnp.int32)
    table = items.reshape(top, rows).T
    table = table[jax.random.permutation(jax.random.fold_in(own, 1), rows)]
    rotation = jax.random.randint(jax.random.fold_in(own, 2), (rows, 1), 0, top)
    return jnp.take_along_axis(table, (jnp.arange(top)[None, :] + rotation) % top, axis=1)


def load_shares(amount, total, reach, lean, full):
    portions = [(1 << 20) // math.isqrt(grade ** lean) + 1 for grade in range(1, amount + 1)]
    largest = reach if full else min(reach, max(-(-total // amount), total * portions[0] // sum(portions)))
    least = 1 if total - largest >= amount - 1 else 0
    given, rest = [largest] + [least] * (amount - 1), total - largest - least * (amount - 1)
    while rest > 0:
        candidates = [i for i in range(1, amount) if given[i] < largest] or [i for i in range(1, amount) if given[i] < reach]
        whole, budget = sum([portions[i] for i in candidates]), rest
        for i in candidates:
            more = min(reach - given[i], max(1, budget * portions[i] // whole), rest)
            given[i] = given[i] + more
            rest = rest - more
    return np.array(given)


def scatter_about(key, extent, deviation, reach, cuts=(), kind=jnp.bfloat16):
    gain = level_of(key, extent, cuts, -0.22, 0.18) if cuts else 1.0
    drawn = jax.random.normal(key, extent, jnp.float32) * deviation * gain
    return jnp.minimum(jnp.maximum(drawn, -reach), reach).astype(kind)


def setup_inputs(seed: int = 0) -> dict:
    streams_of = jax.random.split(jax.random.key(seed), 11)
    tokens = draw_tokens(jax.random.fold_in(streams_of[10], 71), 0)
    norm_gain = jnp.clip(1.0 + 0.18 * jax.random.normal(streams_of[1], (D,), jnp.float32), 0.1, 1.9)
    routes_keys = jax.random.split(jax.random.fold_in(streams_of[2], 1), TOKENS // TOK_DEV)
    routes_turns = jax.random.permutation(jax.random.fold_in(streams_of[2], 3), TOKENS // TOK_DEV)
    routes = jax.vmap(lambda own, number: routed_block(jax.random.fold_in(streams_of[2], 2), own, number, TOK_DEV, EXPERTS, TOPK, CAP, 2))(routes_keys, routes_turns).reshape((TOKENS, TOPK))
    gates = jnp.clip(0.25 + 1.75 * jax.random.uniform(streams_of[3], (TOKENS, TOPK), jnp.float32) ** level_of(streams_of[3], (TOKENS, TOPK), ((0, 32),), -0.2, 0.2), 0.25, 2.0)
    expert_gate = scatter_about(streams_of[4], (EXPERTS, D, EXPERT_UNITS), D ** -0.5, 0.125, ((0, 8),))
    expert_up = scatter_about(streams_of[5], (EXPERTS, D, EXPERT_UNITS), D ** -0.5, 0.125, ((0, 8),))
    expert_down = scatter_about(streams_of[6], (EXPERTS, EXPERT_UNITS, D), EXPERT_UNITS ** -0.5, 0.25, ((0, 8),))
    shared_gate = scatter_about(streams_of[7], (D, SHARED), D ** -0.5, 0.125)
    shared_up = scatter_about(streams_of[8], (D, SHARED), D ** -0.5, 0.125)
    shared_down = scatter_about(streams_of[9], (SHARED, D), SHARED ** -0.5, 0.375)
    return dict(tokens=tokens, norm_gain=norm_gain, routes=routes, gates=gates, expert_gate=expert_gate, expert_up=expert_up, expert_down=expert_down, shared_gate=shared_gate, shared_up=shared_up, shared_down=shared_down)


block_rows = 512

def layer_normed(token_block, norm_gain):
    values = token_block.astype(jnp.float32)
    center = lax.optimization_barrier(jnp.mean(values, axis=-1, keepdims=True))
    spread = lax.optimization_barrier(jnp.mean(jnp.square(values - center), axis=-1, keepdims=True))
    return ((values - center) * lax.rsqrt(spread + 1e-05) * norm_gain).astype(jnp.bfloat16)

def gated_mlp(row_block, w_gate, w_up, w_down):
    gate_part = jnp.dot(row_block, w_gate, preferred_element_type=jnp.float32)
    up_part = jnp.dot(row_block, w_up, preferred_element_type=jnp.float32)
    hidden = (jax.nn.silu(gate_part) * up_part).astype(jnp.bfloat16)
    return jnp.dot(hidden, w_down, preferred_element_type=jnp.float32)

def reference(tokens, norm_gain, routes, gates, expert_gate, expert_up, expert_down, shared_gate, shared_up, shared_down):
    normed = layer_normed(tokens, norm_gain)
    count_rows, feature_count = normed.shape
    copy_count = count_rows * TOPK
    flat_expert = routes.reshape(-1).astype(jnp.int32)
    flat_token = jnp.repeat(jnp.arange(count_rows, dtype=jnp.int32), TOPK)
    sort_order = jnp.argsort(flat_expert, stable=True).astype(jnp.int32)
    sorted_expert = flat_expert[sort_order]
    counts = lax.optimization_barrier(jnp.sum((flat_expert[:, None] == jnp.arange(EXPERTS, dtype=jnp.int32)[None, :]).astype(jnp.int32), axis=0))
    padded = (counts + block_rows - 1) // block_rows * block_rows
    starts = jnp.cumsum(counts) - counts
    block_ends = jnp.cumsum(padded)
    padded_starts = block_ends - padded
    destination = (padded_starts[sorted_expert] + jnp.arange(copy_count, dtype=jnp.int32) - starts[sorted_expert]).astype(jnp.int32)
    block_count = -(-copy_count // block_rows) + EXPERTS
    slot_token = jnp.full((block_count * block_rows,), count_rows, jnp.int32).at[destination].set(flat_token[sort_order])
    block_expert = jnp.clip(jnp.searchsorted(block_ends, jnp.arange(block_count, dtype=jnp.int32) * block_rows, side='right'), 0, EXPERTS - 1).astype(jnp.int32)
    padded_rows = jnp.concatenate([normed, jnp.zeros((1, feature_count), normed.dtype)], axis=0)

    def run_block(block_item):
        slot_tokens, expert = block_item
        row_block = padded_rows[slot_tokens]
        return gated_mlp(row_block, expert_gate[expert], expert_up[expert], expert_down[expert]).astype(jnp.bfloat16)
    slot_out = lax.map(run_block, (slot_token.reshape(block_count, block_rows), block_expert))
    slot_out = slot_out.reshape(block_count * block_rows, feature_count)
    copy_slot = jnp.zeros((copy_count,), jnp.int32).at[sort_order].set(destination).reshape(count_rows, TOPK)
    routed = jnp.zeros((count_rows, feature_count), jnp.float32)
    for choice_index in range(TOPK):
        picked = slot_out[copy_slot[:, choice_index]].astype(jnp.float32)
        routed = routed + gates[:, choice_index][:, None] * picked
    shared_out = gated_mlp(normed, shared_gate, shared_up, shared_down)
    mixed = (routed + shared_out).astype(jnp.bfloat16)
    load = counts.astype(jnp.float32) * (EXPERTS / (count_rows * TOPK))
    return (mixed, load)
```

```python
import functools

import jax
import jax.numpy as jnp
from jax import lax
from jax.experimental import pallas as pl
from jax.experimental.pallas import tpu as pltpu
from jax.sharding import PartitionSpec as P

F32 = jnp.float32
BF16 = jnp.bfloat16


def kernel(
    n,
    eps,
    cap,
    tokens,
    routes,
    gates,
    gain,
    expert_gate,
    expert_up,
    expert_down,
    shared_gate,
    shared_up,
    shared_down,
    out,
    load,
    blocks,
    group_routes,
    every_routes,
    rows_in,
    hidden,
    results,
    returned,
    total,
    w_gate,
    w_up,
    w_down,
    s_gate,
    s_up,
    s_down,
    weight_sem,
    own_sem,
    route_send,
    route_recv,
    far_send,
    far_recv,
    token_send,
    token_recv,
    result_send,
    result_recv,
):
    me = lax.axis_index("tp")
    here = lax.axis_index("ep")
    rows, width = tokens.shape
    half = rows // 2
    chunk = rows // cap
    relay = n == 8
    order = [lax.rem(me + i, n) for i in range(n)]
    if relay:
        core, xbit, ybit = me % 2, (me // 2) % 2, me // 4
        across = 1 - 2 * core
        sib = me + across
        nx = me + 2 * (1 - 2 * xbit)
        ny = me + 4 * (1 - 2 * ybit)
        nd = nx + 4 * (1 - 2 * ybit)
        order = [me, sib, nx, nx + across, ny, ny + across, nd, nd + across]

    weights = [
        pltpu.make_async_copy(src, dst, weight_sem.at[i])
        for i, (src, dst) in enumerate(
            [
                (expert_gate.at[0], w_gate),
                (expert_up.at[0], w_up),
                (expert_down.at[0], w_down),
                (shared_gate, s_gate),
                (shared_up, s_up),
                (shared_down, s_down),
            ]
        )
    ]
    for copy in weights:
        copy.start()
    own_routes = pltpu.make_async_copy(routes, group_routes.at[me], own_sem.at[0])
    own_routes.start()

    barrier = pltpu.get_barrier_semaphore()
    planes = [lax.rem(here + i, eps) for i in range(1, eps)]
    for peer in order[1:]:
        pl.semaphore_signal(barrier, inc=1, device_id={"tp": peer})
    for plane in planes:
        pl.semaphore_signal(barrier, inc=1, device_id={"ep": plane})
    pl.semaphore_wait(barrier, n - 1 + eps - 1)

    pending = []
    for i, peer in enumerate(order[1:]):
        copy = pltpu.make_async_remote_copy(
            src_ref=routes,
            dst_ref=group_routes.at[me],
            send_sem=route_send.at[i],
            recv_sem=route_recv.at[me],
            device_id={"tp": peer},
        )
        copy.start()
        pending.append(copy)

    def part(ref, piece):
        return ref.at[pl.ds(piece * half, half)]

    def send(source, piece, slot, peer, number):
        copy = pltpu.make_async_remote_copy(
            src_ref=part(source, piece),
            dst_ref=part(blocks.at[slot], piece),
            send_sem=token_send.at[number],
            recv_sem=token_recv.at[slot, piece],
            device_id={"tp": peer},
        )
        copy.start()
        pending.append(copy)

    def landed(slot, piece):
        ref = part(blocks.at[slot], piece)
        pltpu.make_async_copy(ref, ref, token_recv.at[slot, piece]).wait()

    if relay:
        send(tokens, 0, me, nx, 0)
        send(tokens, 1, me, ny, 1)
        send(tokens, 1, me, nx, 2)
        send(tokens, 0, me, ny, 3)
        send(tokens, 0, me, sib, 4)
        send(tokens, 1, me, sib, 5)
    else:
        for i, peer in enumerate(order[1:]):
            send(tokens, 0, me, peer, 2 * i)
            send(tokens, 1, me, peer, 2 * i + 1)

    earlier = (
        lax.broadcasted_iota(jnp.int32, (rows, rows), 0)
        < lax.broadcasted_iota(jnp.int32, (rows, rows), 1)
    ).astype(BF16)
    row_in_slot = lax.broadcasted_iota(jnp.int32, (cap, rows), 0)

    def normed_of(values):
        center = jnp.mean(values, axis=-1, keepdims=True)
        values = values - center
        spread = jnp.mean(jnp.square(values), axis=-1, keepdims=True)
        return (values * lax.rsqrt(spread + 1e-05) * gain[...]).astype(BF16)

    def gated(values, gate_ref, up_ref):
        gate_part = jnp.dot(values, gate_ref[...], preferred_element_type=F32)
        up_part = jnp.dot(values, up_ref[...], preferred_element_type=F32)
        return (gate_part * (1.0 / (1.0 + jnp.exp(-gate_part))) * up_part).astype(BF16)

    def gather(number):
        for g in range(chunk):
            source = order[number * chunk + g]
            named = group_routes[source]
            member = (named[0:1] == me) | (named[1:2] == me)
            count = jnp.dot(
                jnp.broadcast_to(member.astype(F32), (8, rows)).astype(BF16),
                earlier,
                preferred_element_type=F32,
            )[0:1].astype(jnp.int32)
            slot = jnp.where(member, count, -1)
            pick = (row_in_slot == slot).astype(F32).astype(BF16)
            held = tokens[...] if number * chunk + g == 0 else blocks[source]
            taken = jnp.dot(pick, held, preferred_element_type=F32)
            rows_in[g * cap : (g + 1) * cap, :] = normed_of(taken)

    tile = 512

    def expert(number):
        hidden[...] = gated(rows_in[...], w_gate, w_up)
        for at in range(0, width, tile):
            value = jnp.dot(
                hidden[...], w_down[:, at : at + tile], preferred_element_type=F32
            ).astype(BF16)
            for g in range(chunk):
                piece = value[g * cap : (g + 1) * cap]
                if number * chunk + g == 0:
                    returned[me, :, at : at + tile] = piece
                else:
                    results[number * chunk + g, :, at : at + tile] = piece
        for g in range(chunk):
            i = number * chunk + g
            if i == 0:
                continue
            copy = pltpu.make_async_remote_copy(
                src_ref=results.at[i],
                dst_ref=returned.at[me],
                send_sem=result_send.at[i],
                recv_sem=result_recv.at[me],
                device_id={"tp": order[i]},
            )
            copy.start()
            pending.append(copy)

    own_routes.wait()
    for peer in order[1:]:
        ref = group_routes.at[peer]
        pltpu.make_async_copy(ref, ref, route_recv.at[peer]).wait()
    for i, plane in enumerate(planes):
        copy = pltpu.make_async_remote_copy(
            src_ref=group_routes,
            dst_ref=every_routes.at[here],
            send_sem=far_send.at[i],
            recv_sem=far_recv.at[here],
            device_id={"ep": plane},
        )
        copy.start()
        pending.append(copy)

    if relay:
        landed(sib, 0)
        landed(sib, 1)
        gather(0)
        landed(nx, 0)
        send(blocks.at[nx], 0, nx, ny, 6)
        send(blocks.at[nx], 0, nx, sib, 7)
        landed(ny, 1)
        send(blocks.at[ny], 1, ny, nx, 8)
        send(blocks.at[ny], 1, ny, sib, 9)
        for copy in weights[:3]:
            copy.wait()
        expert(0)
        landed(nx, 1)
        send(blocks.at[nx], 1, nx, sib, 10)
        landed(ny, 0)
        send(blocks.at[ny], 0, ny, sib, 11)
        for number in (1, 2):
            landed(order[2 * number + 1], 0)
            landed(order[2 * number + 1], 1)
            gather(number)
            expert(number)
        landed(nd, 0)
        send(blocks.at[nd], 0, nd, sib, 12)
        landed(nd, 1)
        send(blocks.at[nd], 1, nd, sib, 13)
        landed(order[7], 0)
        landed(order[7], 1)
        gather(3)
        expert(3)
    else:
        for copy in weights[:3]:
            copy.wait()
        for number in range(n // chunk):
            for source in order[max(1, number * chunk) : (number + 1) * chunk]:
                landed(source, 0)
                landed(source, 1)
            gather(number)
            expert(number)

    for copy in weights[3:]:
        copy.wait()
    rows_in[...] = normed_of(tokens[...].astype(F32))
    shared = gated(rows_in[...], s_gate, s_up)
    for at in range(0, width, tile):
        total[:, at : at + tile] = jnp.dot(
            shared, s_down[:, at : at + tile], preferred_element_type=F32
        )

    expert_ids = lax.broadcasted_iota(jnp.int32, (n, rows), 0)
    first, second = routes[0:1], routes[1:2]
    member = ((first == expert_ids) | (second == expert_ids)).astype(F32)
    ranks = jnp.dot(member.astype(BF16), earlier, preferred_element_type=F32)
    slots = [
        named * cap
        + jnp.sum(jnp.where(named == expert_ids, ranks, 0.0), axis=0, keepdims=True).astype(jnp.int32)
        for named in (first, second)
    ]

    def counted(ref_of, amount, start):
        def step(i, sums):
            named = ref_of(i)
            return (
                sums
                + (named[0:1] == expert_ids).astype(F32)
                + (named[1:2] == expert_ids).astype(F32)
            )

        return lax.fori_loop(0, amount, step, start)

    sums = counted(lambda i: group_routes[i], n, jnp.zeros((n, rows), F32))
    for plane in planes:
        ref = every_routes.at[plane]
        pltpu.make_async_copy(ref, ref, far_recv.at[plane]).wait()
        sums = counted(lambda i, plane=plane: every_routes[plane, i], n, sums)
    counts = lax.dot_general(
        jnp.ones((8, rows), F32),
        sums,
        (((1,), (1,)), ((), ())),
        precision=lax.Precision.HIGHEST,
        preferred_element_type=F32,
    )
    load[...] = counts[0:1, :] * (n / (rows * 2 * n * eps))

    gate_of = [gates[:, k : k + 1] for k in range(2)]
    for number in range(n // chunk):
        sources = order[number * chunk : (number + 1) * chunk]
        for g, source in enumerate(sources):
            if number * chunk + g > 0:
                ref = returned.at[source]
                pltpu.make_async_copy(ref, ref, result_recv.at[source]).wait()
        picks = [
            jnp.transpose(
                jnp.concatenate(
                    [(row_in_slot + source * cap == slot).astype(F32) for source in sources], axis=0
                )
            ).astype(BF16)
            for slot in slots
        ]
        last = number == n // chunk - 1
        for at in range(0, width, tile):
            back = jnp.concatenate([returned[source, :, at : at + tile] for source in sources], axis=0)
            value = total[:, at : at + tile]
            for k in range(2):
                value = value + gate_of[k] * jnp.dot(picks[k], back, preferred_element_type=F32)
            if last:
                out[:, at : at + tile] = value.astype(BF16)
            else:
                total[:, at : at + tile] = value

    for copy in pending:
        copy.wait_send()


def per_device(
    tokens,
    norm_gain,
    routes,
    gates,
    expert_gate,
    expert_up,
    expert_down,
    shared_gate,
    shared_up,
    shared_down,
):
    n, eps = lax.axis_size("tp"), lax.axis_size("ep")
    rows, width = tokens.shape
    top = routes.shape[1]
    cap = 2 * rows * top // n
    units = expert_gate.shape[2]
    sends = 14 if n == 8 else 2 * (n - 1)
    vmem = pl.BlockSpec(memory_space=pltpu.VMEM)
    hbm = pl.BlockSpec(memory_space=pl.ANY)
    dma = pltpu.SemaphoreType.DMA
    mixed, load = pl.pallas_call(
        functools.partial(kernel, n, eps, cap),
        out_shape=(
            jax.ShapeDtypeStruct((rows, width), BF16),
            jax.ShapeDtypeStruct((1, n), F32),
        ),
        in_specs=[vmem] * 4 + [hbm] * 6,
        out_specs=(vmem, vmem),
        scratch_shapes=[
            pltpu.VMEM((n, rows, width), BF16),
            pltpu.VMEM((n, top, rows), jnp.int32),
            pltpu.VMEM((eps, n, top, rows), jnp.int32),
            pltpu.VMEM((rows, width), BF16),
            pltpu.VMEM((rows, units), BF16),
            pltpu.VMEM((n, cap, width), BF16),
            pltpu.VMEM((n, cap, width), BF16),
            pltpu.VMEM((rows, width), F32),
            pltpu.VMEM(expert_gate.shape[1:], BF16),
            pltpu.VMEM(expert_up.shape[1:], BF16),
            pltpu.VMEM(expert_down.shape[1:], BF16),
            pltpu.VMEM(shared_gate.shape, BF16),
            pltpu.VMEM(shared_up.shape, BF16),
            pltpu.VMEM(shared_down.shape, BF16),
            dma((6,)),
            dma((1,)),
            dma((n - 1,)),
            dma((n,)),
            dma((max(1, eps - 1),)),
            dma((eps,)),
            dma((sends,)),
            dma((n, 2)),
            dma((n,)),
            dma((n,)),
        ],
        compiler_params=pltpu.CompilerParams(collective_id=0, has_side_effects=True),
    )(
        tokens,
        routes.T,
        gates,
        norm_gain.reshape(1, width),
        expert_gate,
        expert_up,
        expert_down,
        shared_gate,
        shared_up,
        shared_down,
    )
    return mixed, load.reshape(n)


def solution(mesh):
    placed = (
        P(("ep", "tp"), None),
        P(),
        P(("ep", "tp"), None),
        P(("ep", "tp"), None),
        P("tp", None, None),
        P("tp", None, None),
        P("tp", None, None),
        P(),
        P(),
        P(),
    )
    return jax.shard_map(
        per_device,
        mesh=mesh,
        in_specs=placed,
        out_specs=(P(("ep", "tp"), None), P()),
        check_vma=False,
    )
```

```python
import functools

import jax
import jax.numpy as jnp
from jax import lax
from jax.experimental import pallas as pl
from jax.experimental.pallas import tpu as pltpu
from jax.sharding import PartitionSpec as P

F32 = jnp.float32
BF16 = jnp.bfloat16


def kernel(
    n,
    eps,
    cap,
    tokens_hbm,
    routes,
    gates,
    gain,
    expert_gate,
    expert_up,
    expert_down,
    shared_gate,
    shared_up,
    shared_down,
    out,
    load,
    tokens,
    blocks,
    group_routes,
    every_routes,
    rows_in,
    hidden,
    results,
    returned,
    total,
    w_gate,
    w_up,
    w_down,
    s_gate,
    s_up,
    s_down,
    weight_sem,
    own_sem,
    route_send,
    route_recv,
    far_send,
    far_recv,
    token_send,
    token_recv,
    result_send,
    result_recv,
):
    me = lax.axis_index("tp")
    here = lax.axis_index("ep")
    rows, width = tokens.shape
    half = rows // 2
    chunk = rows // cap
    relay = n == 8
    order = [lax.rem(me + i, n) for i in range(n)]
    if relay:
        core, xbit, ybit = me % 2, (me // 2) % 2, me // 4
        across = 1 - 2 * core
        sib = me + across
        nx = me + 2 * (1 - 2 * xbit)
        ny = me + 4 * (1 - 2 * ybit)
        nd = nx + 4 * (1 - 2 * ybit)
        order = [me, sib, nx, nx + across, ny, ny + across, nd, nd + across]

    barrier = pltpu.get_barrier_semaphore()
    planes = [lax.rem(here + i, eps) for i in range(1, eps)]
    for peer in order[1:]:
        pl.semaphore_signal(barrier, inc=1, device_id={"tp": peer})
    for plane in planes:
        pl.semaphore_signal(barrier, inc=1, device_id={"ep": plane})
    own_tokens = pltpu.make_async_copy(tokens_hbm, tokens, own_sem.at[1])
    own_tokens.start()

    weights = [
        pltpu.make_async_copy(src, dst, weight_sem.at[i])
        for i, (src, dst) in enumerate(
            [
                (expert_gate.at[0], w_gate),
                (expert_up.at[0], w_up),
                (expert_down.at[0], w_down),
                (shared_gate, s_gate),
                (shared_up, s_up),
                (shared_down, s_down),
            ]
        )
    ]
    for copy in weights:
        copy.start()
    own_routes = pltpu.make_async_copy(routes, group_routes.at[me], own_sem.at[0])
    own_routes.start()

    pl.semaphore_wait(barrier, n - 1 + eps - 1)

    pending = []
    for i, peer in enumerate(order[1:]):
        copy = pltpu.make_async_remote_copy(
            src_ref=routes,
            dst_ref=group_routes.at[me],
            send_sem=route_send.at[i],
            recv_sem=route_recv.at[me],
            device_id={"tp": peer},
        )
        copy.start()
        pending.append(copy)

    def part(ref, piece):
        return ref.at[pl.ds(piece * half, half)]

    def send(source, piece, slot, peer, number):
        copy = pltpu.make_async_remote_copy(
            src_ref=part(source, piece),
            dst_ref=part(blocks.at[slot], piece),
            send_sem=token_send.at[number],
            recv_sem=token_recv.at[slot, piece],
            device_id={"tp": peer},
        )
        copy.start()
        pending.append(copy)

    def landed(slot, piece):
        ref = part(blocks.at[slot], piece)
        pltpu.make_async_copy(ref, ref, token_recv.at[slot, piece]).wait()

    own_tokens.wait()
    if relay:
        send(tokens, 0, me, nx, 0)
        send(tokens, 1, me, ny, 1)
        send(tokens, 1, me, nx, 2)
        send(tokens, 0, me, ny, 3)
        send(tokens, 0, me, sib, 4)
        send(tokens, 1, me, sib, 5)
    else:
        for i, peer in enumerate(order[1:]):
            send(tokens, 0, me, peer, 2 * i)
            send(tokens, 1, me, peer, 2 * i + 1)

    earlier = (
        lax.broadcasted_iota(jnp.int32, (rows, rows), 0)
        < lax.broadcasted_iota(jnp.int32, (rows, rows), 1)
    ).astype(BF16)
    row_in_slot = lax.broadcasted_iota(jnp.int32, (cap, rows), 0)

    def normed_of(values):
        center = jnp.mean(values, axis=-1, keepdims=True)
        values = values - center
        spread = jnp.mean(jnp.square(values), axis=-1, keepdims=True)
        return (values * lax.rsqrt(spread + 1e-05) * gain[...]).astype(BF16)

    def gated(values, gate_ref, up_ref):
        gate_part = jnp.dot(values, gate_ref[...], preferred_element_type=F32)
        up_part = jnp.dot(values, up_ref[...], preferred_element_type=F32)
        return (gate_part * (1.0 / (1.0 + jnp.exp(-gate_part))) * up_part).astype(BF16)

    def gather(i, at):
        source = order[i]
        named = group_routes[source]
        member = (named[0:1] == me) | (named[1:2] == me)
        count = jnp.dot(
            jnp.broadcast_to(member.astype(F32), (8, rows)).astype(BF16),
            earlier,
            preferred_element_type=F32,
        )[0:1].astype(jnp.int32)
        slot = jnp.where(member, count, -1)
        pick = (row_in_slot == slot).astype(F32).astype(BF16)
        held = tokens[...] if i == 0 else blocks[source]
        taken = jnp.dot(pick, held, preferred_element_type=F32)
        rows_in[at * cap : (at + 1) * cap, :] = normed_of(taken)

    tile = 512

    def expert(members):
        count = len(members) * cap
        hidden[:count] = gated(rows_in[:count], w_gate, w_up)
        for at in range(0, width, tile):
            value = jnp.dot(
                hidden[:count], w_down[:, at : at + tile], preferred_element_type=F32
            ).astype(BF16)
            for g, i in enumerate(members):
                piece = value[g * cap : (g + 1) * cap]
                if i == 0:
                    returned[me, :, at : at + tile] = piece
                else:
                    results[i, :, at : at + tile] = piece
        for i in members:
            if i == 0:
                continue
            copy = pltpu.make_async_remote_copy(
                src_ref=results.at[i],
                dst_ref=returned.at[me],
                send_sem=result_send.at[i],
                recv_sem=result_recv.at[me],
                device_id={"tp": order[i]},
            )
            copy.start()
            pending.append(copy)

    own_routes.wait()
    for peer in order[1:]:
        ref = group_routes.at[peer]
        pltpu.make_async_copy(ref, ref, route_recv.at[peer]).wait()
    for i, plane in enumerate(planes):
        copy = pltpu.make_async_remote_copy(
            src_ref=group_routes,
            dst_ref=every_routes.at[here],
            send_sem=far_send.at[i],
            recv_sem=far_recv.at[here],
            device_id={"ep": plane},
        )
        copy.start()
        pending.append(copy)

    if relay:
        gather(0, 0)
        landed(sib, 0)
        landed(sib, 1)
        gather(1, 1)
        landed(nx, 0)
        send(blocks.at[nx], 0, nx, ny, 6)
        send(blocks.at[nx], 0, nx, sib, 7)
        landed(ny, 1)
        send(blocks.at[ny], 1, ny, nx, 8)
        send(blocks.at[ny], 1, ny, sib, 9)
        for copy in weights[:3]:
            copy.wait()
        expert([0, 1])
        landed(nx, 1)
        send(blocks.at[nx], 1, nx, sib, 10)
        landed(ny, 0)
        send(blocks.at[ny], 0, ny, sib, 11)
        gather(2, 0)
        gather(4, 1)
        expert([2, 4])
        for i, at in ((3, 0), (5, 1)):
            landed(order[i], 0)
            landed(order[i], 1)
            gather(i, at)
        expert([3, 5])
        landed(nd, 0)
        send(blocks.at[nd], 0, nd, sib, 12)
        landed(nd, 1)
        send(blocks.at[nd], 1, nd, sib, 13)
        gather(6, 0)
        landed(order[7], 0)
        landed(order[7], 1)
        gather(7, 1)
        expert([6, 7])
    else:
        for copy in weights[:3]:
            copy.wait()
        for number in range(n // chunk):
            members = list(range(number * chunk, (number + 1) * chunk))
            for i in members:
                if i > 0:
                    landed(order[i], 0)
                    landed(order[i], 1)
                gather(i, i % chunk)
            expert(members)

    for copy in weights[3:]:
        copy.wait()
    rows_in[:rows] = normed_of(tokens[...].astype(F32))
    shared = gated(rows_in[:rows], s_gate, s_up)
    for at in range(0, width, tile):
        total[:, at : at + tile] = jnp.dot(
            shared, s_down[:, at : at + tile], preferred_element_type=F32
        )

    expert_ids = lax.broadcasted_iota(jnp.int32, (n, rows), 0)
    first, second = routes[0:1], routes[1:2]
    member = ((first == expert_ids) | (second == expert_ids)).astype(F32)
    ranks = jnp.dot(member.astype(BF16), earlier, preferred_element_type=F32)
    slots = [
        named * cap
        + jnp.sum(jnp.where(named == expert_ids, ranks, 0.0), axis=0, keepdims=True).astype(jnp.int32)
        for named in (first, second)
    ]

    def counted(ref_of, amount, start):
        def step(i, sums):
            named = ref_of(i)
            return (
                sums
                + (named[0:1] == expert_ids).astype(F32)
                + (named[1:2] == expert_ids).astype(F32)
            )

        return lax.fori_loop(0, amount, step, start)

    sums = counted(lambda i: group_routes[i], n, jnp.zeros((n, rows), F32))
    for plane in planes:
        ref = every_routes.at[plane]
        pltpu.make_async_copy(ref, ref, far_recv.at[plane]).wait()
        sums = counted(lambda i, plane=plane: every_routes[plane, i], n, sums)
    counts = lax.dot_general(
        jnp.ones((8, rows), F32),
        sums,
        (((1,), (1,)), ((), ())),
        precision=lax.Precision.HIGHEST,
        preferred_element_type=F32,
    )
    load[...] = counts[0:1, :] * (n / (rows * 2 * n * eps))

    columns = jnp.transpose(jnp.broadcast_to(gates[0:1], (8, rows))), jnp.transpose(
        jnp.broadcast_to(gates[1:2], (8, rows))
    )
    gate_of = [column[:, 0:1] for column in columns]
    if relay:
        parts = [[0, 1], [2, 4], [3, 5], [6], [7]]
    else:
        parts = [list(range(at, at + chunk)) for at in range(0, n, chunk)]
    for members in parts:
        sources = [order[i] for i in members]
        picks = [
            jnp.transpose(
                jnp.concatenate(
                    [(row_in_slot + source * cap == slot).astype(F32) for source in sources], axis=0
                )
            ).astype(BF16)
            for slot in slots
        ]
        for i, source in zip(members, sources):
            if i > 0:
                ref = returned.at[source]
                pltpu.make_async_copy(ref, ref, result_recv.at[source]).wait()
        last = members is parts[-1]
        for at in range(0, width, tile):
            back = jnp.concatenate([returned[source, :, at : at + tile] for source in sources], axis=0)
            value = total[:, at : at + tile]
            for k in range(2):
                value = value + gate_of[k] * jnp.dot(picks[k], back, preferred_element_type=F32)
            if last:
                out[:, at : at + tile] = value.astype(BF16)
            else:
                total[:, at : at + tile] = value

    for copy in pending:
        copy.wait_send()


def write_out(mixed, load, mixed_out, load_out, sem):
    copies = [
        pltpu.make_async_copy(mixed, mixed_out, sem.at[0]),
        pltpu.make_async_copy(load, load_out, sem.at[1]),
    ]
    for copy in copies:
        copy.start()
    for copy in copies:
        copy.wait()


def per_device(
    tokens,
    norm_gain,
    routes,
    gates,
    expert_gate,
    expert_up,
    expert_down,
    shared_gate,
    shared_up,
    shared_down,
):
    n, eps = lax.axis_size("tp"), lax.axis_size("ep")
    rows, width = tokens.shape
    top = routes.shape[1]
    cap = 2 * rows * top // n
    units = expert_gate.shape[2]
    sends = 14 if n == 8 else 2 * (n - 1)
    vmem = pl.BlockSpec(memory_space=pltpu.VMEM)
    hbm = pl.BlockSpec(memory_space=pl.ANY)
    dma = pltpu.SemaphoreType.DMA
    mixed, load = pl.pallas_call(
        functools.partial(kernel, n, eps, cap),
        out_shape=(
            pltpu.VMEM((rows, width), BF16),
            pltpu.VMEM((1, n), F32),
        ),
        in_specs=[hbm] + [vmem] * 3 + [hbm] * 6,
        out_specs=(vmem, vmem),
        scratch_shapes=[
            pltpu.VMEM((rows, width), BF16),
            pltpu.VMEM((n, rows, width), BF16),
            pltpu.VMEM((n, top, rows), jnp.int32),
            pltpu.VMEM((eps, n, top, rows), jnp.int32),
            pltpu.VMEM((rows, width), BF16),
            pltpu.VMEM((rows, units), BF16),
            pltpu.VMEM((n, cap, width), BF16),
            pltpu.VMEM((n, cap, width), BF16),
            pltpu.VMEM((rows, width), F32),
            pltpu.VMEM(expert_gate.shape[1:], BF16),
            pltpu.VMEM(expert_up.shape[1:], BF16),
            pltpu.VMEM(expert_down.shape[1:], BF16),
            pltpu.VMEM(shared_gate.shape, BF16),
            pltpu.VMEM(shared_up.shape, BF16),
            pltpu.VMEM(shared_down.shape, BF16),
            dma((6,)),
            dma((2,)),
            dma((n - 1,)),
            dma((n,)),
            dma((max(1, eps - 1),)),
            dma((eps,)),
            dma((sends,)),
            dma((n, 2)),
            dma((n,)),
            dma((n,)),
        ],
        compiler_params=pltpu.CompilerParams(
            collective_id=0, has_side_effects=True
        ),
    )(
        tokens,
        routes.T,
        gates.T,
        norm_gain.reshape(1, width),
        expert_gate,
        expert_up,
        expert_down,
        shared_gate,
        shared_up,
        shared_down,
    )
    mixed, load = pl.pallas_call(
        write_out,
        out_shape=(
            jax.ShapeDtypeStruct((rows, width), BF16),
            jax.ShapeDtypeStruct((1, n), F32),
        ),
        in_specs=[vmem] * 2,
        out_specs=(hbm, hbm),
        scratch_shapes=[dma((2,))],
        compiler_params=pltpu.CompilerParams(vmem_limit_bytes=1 << 20),
    )(mixed, load)
    return mixed, load.reshape(n)


def solution(mesh):
    placed = (
        P(("ep", "tp"), None),
        P(),
        P(("ep", "tp"), None),
        P(("ep", "tp"), None),
        P("tp", None, None),
        P("tp", None, None),
        P("tp", None, None),
        P(),
        P(),
        P(),
    )
    return jax.shard_map(
        per_device,
        mesh=mesh,
        in_specs=placed,
        out_specs=(P(("ep", "tp"), None), P()),
        check_vma=False,
    )
```
